256 devices in a mesh: sp: 32 (over z, y), tp: 8 (over x, core).
Axes of the slice: x: 4, y: 4, z: 8, core: 2. Of those that a mesh axis runs over, the one named last changes fastest.
Arguments:
- residual_in: bfloat16 [12288, 2048], P(('sp', 'tp')), may hold values from -6 to 6
- queries: bfloat16 [12288, 2048], P('sp', 'tp'), may hold values from -180 to 180
- keys: bfloat16 [12288, 2048], P('sp', 'tp'), may hold values from -9 to 9
- values: bfloat16 [12288, 2048], P('sp', 'tp'), may hold values from -6 to 6
- mix_lambda: float32 [16], P('tp'), may hold values from 0.3 to 0.8
- head_gain: float32 [128], replicated, may hold values from 0.1 to 1.9
- out_weight: bfloat16 [2048, 2048], P('tp'), may hold values from -0.125 to 0.125
- norm_gain: float32 [2048], replicated, may hold values from 0.1 to 1.9
- gate_weight: bfloat16 [2048, 5632], P('sp', 'tp'), may hold values from -0.125 to 0.125
- up_weight: bfloat16 [2048, 5632], P('sp', 'tp'), may hold values from -0.125 to 0.125
- down_weight: bfloat16 [5632, 2048], P('tp', 'sp'), may hold values from -0.078125 to 0.078125
Outputs:
- layer_out: bfloat16 [12288, 2048], P(('sp', 'tp'))
The draws below stay inside these ranges and needn't reach their ends.
All inputs are finite; a program needn't handle non-finite values.
Results may differ from the reference program's by a relative error of at most 0.014.
Values may be sent and summed in bfloat16 or wider, within the bound.
A program may use at most 128 MiB of HBM per device.

```python
import math
import jax
import jax.numpy as jnp
from jax import lax

D = 2048
H = 16
DH = 64
VD = 128
FF = 5632
TOKENS = 12288


def shared_keys(key):
    base = jax.random.fold_in(key, 101)
    drawn = jnp.clip(1.3 * jax.random.normal(jax.random.fold_in(base, 1), (TOKENS, H * 2 * DH), jnp.float32), -8.0, 8.0)
    return drawn


def draw_keys(key, part):
    drawn = shared_keys(key)
    return drawn.astype(jnp.bfloat16)


def draw_queries(key, part):
    base = jax.random.fold_in(key, 202)
    drawn = jnp.clip(1.3 * jax.random.normal(jax.random.fold_in(base, 1), (TOKENS, H * 2 * DH), jnp.float32), -8.0, 8.0)
    return drawn.astype(jnp.bfloat16)


def block_levels(own_key, dims, shards, low, largest):
    loudness, own = 1.0, jax.random.fold_in(own_key, 6)
    for position, parts in shards:
        heights = jnp.exp(jax.random.uniform(jax.random.fold_in(own, position), (parts,), jnp.float32, low / len(shards), largest / len(shards)))
        loudness = loudness * jnp.repeat(heights, dims[position] // parts).reshape([-1 if axis == position else 1 for axis in range(len(dims))])
    return loudness


def bell_draw(key, extent, width, limit, cuts=(), kind=jnp.bfloat16):
    values = jax.random.normal(key, extent, jnp.float32) * width
    if len(cuts) > 0:
        values = block_levels(key, extent, cuts, -0.22, 0.18) * values
    return jnp.clip(values, min=-limit, max=limit).astype(kind)


def setup_inputs(seed: int = 0) -> dict:
    arg_keys = jax.random.split(jax.random.key(seed), 12)
    return {
        "residual_in": bell_draw(arg_keys[0], (TOKENS, D), 1.0, 6.0, ((0, 256),)),
        "queries": draw_queries(jax.random.fold_in(arg_keys[11], 71), 0),
        "keys": draw_keys(jax.random.fold_in(arg_keys[11], 71), 0),
        "values": bell_draw(arg_keys[3], (TOKENS, H * VD), 1.0, 6.0, ((0, 32), (1, 8))),
        "mix_lambda": jnp.clip(0.3 + 0.5 * jax.random.uniform(arg_keys[4], (H,), jnp.float32) ** block_levels(arg_keys[4], (H,), ((0, 8),), -0.2, 0.2), 0.3, 0.8),
        "head_gain": jnp.clip(1.0 + 0.18 * jax.random.normal(arg_keys[5], (VD,), jnp.float32), 0.1, 1.9),
        "out_weight": bell_draw(arg_keys[6], (H * VD, D), (H * VD) ** -0.5, 0.125, ((0, 8),)),
        "norm_gain": jnp.clip(1.0 + 0.18 * jax.random.normal(arg_keys[7], (D,), jnp.float32), 0.1, 1.9),
        "gate_weight": bell_draw(arg_keys[8], (D, FF), D ** -0.5, 0.125, ((0, 32), (1, 8))),
        "up_weight": bell_draw(arg_keys[9], (D, FF), D ** -0.5, 0.125, ((0, 32), (1, 8))),
        "down_weight": bell_draw(arg_keys[10], (FF, D), FF ** -0.5, 0.078125, ((0, 8), (1, 32))),
    }


def head_rows(args):
    query_head, key_head, value_head, weight_two, head_gain = args
    block_rows = math.gcd(512, TOKENS)
    blocks = query_head.reshape(TOKENS // block_rows, block_rows, 2, DH)
    key_float = key_head.astype(jnp.float32)
    value_float = value_head.astype(jnp.float32)

    def one_block(query_block):
        scores = jnp.einsum('qcd,kcd->cqk', query_block.astype(jnp.float32), key_float) / math.sqrt(DH)
        top = lax.optimization_barrier(jnp.max(scores, axis=-1, keepdims=True))
        expo = jnp.exp(scores - top)
        total = lax.optimization_barrier(jnp.sum(expo, axis=-1, keepdims=True))
        probs = lax.optimization_barrier(expo.astype(jnp.bfloat16)).astype(jnp.float32)
        maps = jnp.einsum('cqk,ke->cqe', probs, value_float) / total
        mixed = maps[0] - weight_two * maps[1]
        scale = lax.rsqrt(lax.optimization_barrier(jnp.mean(mixed * mixed, axis=-1, keepdims=True)) + 1e-06)
        return (mixed * scale * head_gain).astype(jnp.bfloat16)
    return lax.map(one_block, blocks).reshape(TOKENS, VD)

def reference(residual_in, queries, keys, values, mix_lambda, head_gain, out_weight, norm_gain, gate_weight, up_weight, down_weight):
    query_heads = jnp.transpose(queries.reshape(TOKENS, H, 2, DH), (1, 0, 2, 3))
    key_heads = jnp.transpose(keys.reshape(TOKENS, H, 2, DH), (1, 0, 2, 3))
    value_heads = jnp.transpose(values.reshape(TOKENS, H, VD), (1, 0, 2))
    gains = jnp.broadcast_to(head_gain, (H, VD))
    per_head = lax.map(head_rows, (query_heads, key_heads, value_heads, mix_lambda, gains))
    attended = jnp.transpose(per_head, (1, 0, 2)).reshape(TOKENS, H * VD)
    after_mix = residual_in.astype(jnp.float32) + jnp.dot(attended, out_weight, preferred_element_type=jnp.float32)
    scale = lax.rsqrt(lax.optimization_barrier(jnp.mean(after_mix * after_mix, axis=-1, keepdims=True)) + 1e-06)
    normed = (after_mix * scale * norm_gain).astype(jnp.bfloat16)
    gate = jnp.dot(normed, gate_weight, preferred_element_type=jnp.float32)
    up = jnp.dot(normed, up_weight, preferred_element_type=jnp.float32)
    hidden = (jax.nn.silu(gate) * up).astype(jnp.bfloat16)
    mixer = jnp.dot(hidden, down_weight, preferred_element_type=jnp.float32)
    return (after_mix + 0.5 * mixer).astype(jnp.bfloat16)
```

```python
import math

import jax
import jax.numpy as jnp
from jax import lax
from jax.experimental import pallas as pl
from jax.experimental.pallas import tpu as pltpu
from jax.sharding import PartitionSpec as P

MESH = pl.DeviceIdType.MESH
F32 = jnp.float32
BF16 = jnp.bfloat16

TB = 384
VD = 128
D = 2048
FL = 704
WC = 3 * FL
OWN = 48
SCALE = math.log2(math.e) / 8.0


class Link:
    def __init__(self, send, recv):
        self.send, self.recv, self.count, self.live = send, recv, 0, []

    def copy(self, src, dst, dev):
        k = self.count
        self.count += 1
        return pltpu.make_async_remote_copy(
            src_ref=src,
            dst_ref=dst,
            send_sem=self.send.at[k],
            recv_sem=self.recv.at[k],
            device_id=dev,
            device_id_type=MESH,
        )

    def start(self, src, dst, dev):
        c = self.copy(src, dst, dev)
        c.start()
        self.live.append(c)
        return c

    def finish(self):
        for c in self.live:
            c.wait_send()


def places():
    sp, tp = lax.axis_index("sp"), lax.axis_index("tp")
    z, y = sp // 4, sp % 4
    x, c = tp // 2, tp % 2

    def at(dz=0, dy=0, dx=0, other=False):
        nz, ny, nx = (z + dz + 8) % 8, (y + dy + 4) % 4, (x + dx + 4) % 4
        nc = 1 - c if other else c
        return (nz * 4 + ny, nx * 2 + nc)

    return z, y, x, c, at


def meet(peers):
    barrier = pltpu.get_barrier_semaphore()
    for dev in peers:
        pl.semaphore_signal(barrier, inc=1, device_id=dev, device_id_type=MESH)
    pl.semaphore_wait(barrier, len(peers))


def half(ref, k):
    w = ref.shape[-1] // 2
    return ref.at[:, pl.ds(k * w, w)]


class Gather4:
    def __init__(self, link, buf, left, right):
        self.link, self.buf, self.left, self.right = link, buf, left, right

    def begin(self):
        b = self.buf
        self.r1 = self.link.start(b.at[0], b.at[1], self.right)
        self.l1 = self.link.start(b.at[0], b.at[2], self.left)

    def near(self):
        b = self.buf
        self.r1.wait_recv()
        self.r2 = self.link.start(half(b.at[1], 0), half(b.at[3], 0), self.right)
        self.l1.wait_recv()
        self.l2 = self.link.start(half(b.at[2], 1), half(b.at[3], 1), self.left)

    def far(self):
        self.r2.wait_recv()
        self.l2.wait_recv()


class Reduce4:
    def __init__(self, link, part, land, left, right):
        self.link, self.part, self.land, self.left, self.right = link, part, land, left, right

    def begin(self, k):
        p, t = self.part, self.land
        dev, near = (self.right, self.left) if k == 0 else (self.left, self.right)
        far = self.link.start(half(p.at[3], k), half(t.at[2], k), dev)
        if k == 0:
            self.far0, self.direct0 = far, self.link.start(half(p.at[1], 0), half(t.at[1], 0), near)
        else:
            self.far1, self.direct1 = far, self.link.start(half(p.at[2], 1), half(t.at[0], 1), near)

    def pass_on(self, k):
        p, t = self.part, self.land
        w = p.shape[-1] // 2
        cols = slice(k * w, (k + 1) * w)
        (self.far0 if k == 0 else self.far1).wait_recv()
        slot = 2 if k == 0 else 1
        p[slot, :, cols] = (p[slot, :, cols].astype(F32) + t[2, :, cols].astype(F32)).astype(BF16)
        if k == 0:
            self.sum0 = self.link.start(half(p.at[2], 0), half(t.at[0], 0), self.right)
        else:
            self.sum1 = self.link.start(half(p.at[1], 1), half(t.at[1], 1), self.left)

    def end(self, k):
        (self.direct0 if k == 0 else self.direct1).wait_recv()
        (self.sum0 if k == 0 else self.sum1).wait_recv()


def attend(qst, acc, top, h, keys, lo, hi):
    n = keys.shape[0]
    sub = TB // 2

    def step(i, carry):
        kk = keys[:, :VD]
        ve = jnp.concatenate([keys[:, VD:], jnp.ones((n, VD), BF16)], axis=1)
        for j in range(2):
            r = pl.ds(j * sub, sub)
            s = lax.dot_general(
                qst[h, i, r, :], kk, (((1,), (1,)), ((), ())), preferred_element_type=F32
            )
            old = top[h, i, r, :]
            new = jnp.maximum(old, jnp.max(s, axis=1, keepdims=True))
            alpha = jnp.exp2((old - new) * SCALE)
            wide = jnp.concatenate([new] * (n // VD), axis=1)
            p = jnp.exp2((s - wide) * SCALE).astype(BF16)
            o = jnp.dot(p, ve, preferred_element_type=F32)
            acc[h, i, r, :] = acc[h, i, r, :] * jnp.concatenate([alpha, alpha], axis=1) + o
            top[h, i, r, :] = new
        return carry

    lax.fori_loop(2 * lo, 2 * hi, step, 0)


def split_queries(qbuf, qst, slot):
    lane = lax.broadcasted_iota(jnp.int32, (TB, VD), 1)
    for h in range(2):
        q = qbuf[slot, :, h * VD : (h + 1) * VD]
        zero = jnp.zeros_like(q)
        qst[h, 2 * slot, :, :] = jnp.where(lane < 64, q, zero)
        qst[h, 2 * slot + 1, :, :] = jnp.where(lane < 64, zero, q)


def gather_stats(acc, top, stat, h):
    lane = lax.broadcasted_iota(jnp.int32, (VD, VD), 1)
    mat = jnp.zeros((VD, VD), F32)
    for i in range(8):
        for j in range(3):
            g = (i // 2) * 8 + (i % 2) * 3 + j
            r = slice(j * VD, (j + 1) * VD)
            mat = jnp.where(lane == g, top[h, i, r, :], mat)
            mat = jnp.where(lane == g + 32, acc[h, i, r, VD:], mat)
    stat[h] = jnp.transpose(mat)[:64]


SLOTS = ((1, 3, 0, 2), (2, 0, 3, 1), (3, 2, 1, 0))


def blend(acc, stat, got, lam, part, mine, h):
    def of(ref, p, base):
        if p is None:
            return ref[h, base : base + 32, :]
        return jnp.concatenate([ref[p, h, base + 8 * s : base + 8 * s + 8, :] for s in SLOTS[p]])

    tops = [of(stat, None, 0)] + [of(got, p, 0) for p in range(3)]
    sums = [of(stat, None, 32)] + [of(got, p, 32) for p in range(3)]
    top = jnp.maximum(jnp.maximum(tops[0], tops[1]), jnp.maximum(tops[2], tops[3]))
    weights = [jnp.exp2((t - top) * SCALE) for t in tops]
    total = sum(w * s for w, s in zip(weights, sums))
    row = lax.broadcasted_iota(jnp.int32, (32, VD), 0) % 8
    sign = jnp.where(row < 3, 1.0, -lam[h])
    factor = sign * weights[0] / jnp.where(row < 6, total, 1.0)
    turned = jnp.transpose(jnp.concatenate([factor, jnp.zeros((96, VD), F32)]))
    cols = slice(h * VD, (h + 1) * VD)
    for s in range(4):
        for j in range(3):
            r = slice(j * VD, (j + 1) * VD)
            g = 8 * s + j
            m = (
                acc[h, 2 * s, r, :VD] * turned[:, g : g + 1]
                + acc[h, 2 * s + 1, r, :VD] * turned[:, g + 3 : g + 4]
            )
            if s == 0:
                mine[r, cols] = m
            else:
                part[s, r, cols] = m.astype(BF16)


def front_kernel(
    q_hbm, k_hbm, v_hbm, res_ref, ow_ref, lam_ref, gain_ref, ngain_ref,
    rows_ref, mix_ref,
    qbuf, qst, kvo, kvp, kvf, acc, top, stat, got, part, land, mine,
    att, attr, px, dsend, drecv, pxb, land2, lsem, send, recv,
):
    z, y, x, c, at = places()
    zr, zl, yr, yl, yf = at(dz=1), at(dz=-1), at(dy=1), at(dy=-1), at(dy=2)
    xr, xl, other = at(dx=1), at(dx=-1), at(other=True)
    loads = [pltpu.make_async_copy(q_hbm, qbuf.at[0], lsem.at[0])]
    for h in range(2):
        cols = pl.ds(h * VD, VD)
        loads.append(pltpu.make_async_copy(k_hbm.at[:, cols], kvo.at[h, :, pl.ds(0, VD)], lsem.at[1 + h]))
        loads.append(pltpu.make_async_copy(v_hbm.at[:, cols], kvo.at[h, :, pl.ds(VD, VD)], lsem.at[3 + h]))
    for l in loads:
        l.start()
    link = Link(send, recv)
    acc[...] = jnp.zeros_like(acc)
    top[...] = jnp.full_like(top, -1e30)
    for l in loads:
        l.wait()
    meet((zr, zl, yr, yl, yf, xr, xl, other))

    qg = Gather4(link, qbuf, yl, yr)
    qg.begin()
    from_l, from_r = [None, None], [None, None]
    for h in range(2):
        from_l[h] = link.start(kvo.at[h], kvp.at[0, h, 0], zr)
        from_r[h] = link.start(kvo.at[h], kvp.at[0, h, 1], zl)

    def forward(s, h):
        from_l[h].wait_recv()
        if s < 2:
            nl = link.start(kvp.at[s, h, 0], kvp.at[s + 1, h, 0], zr)
        else:
            nl = link.start(kvp.at[s, h, 0, pl.ds(0, TB // 2)], kvf.at[h, pl.ds(0, TB // 2)], zr)
        from_r[h].wait_recv()
        if s < 2:
            nr = link.start(kvp.at[s, h, 1], kvp.at[s + 1, h, 1], zl)
        else:
            nr = link.start(kvp.at[s, h, 1, pl.ds(TB // 2, TB // 2)], kvf.at[h, pl.ds(TB // 2, TB // 2)], zl)
        from_l[h], from_r[h] = nl, nr

    split_queries(qbuf, qst, 0)
    for h in range(2):
        attend(qst, acc, top, h, kvo.at[h], 0, 1)
    qg.near()
    forward(0, 0)
    split_queries(qbuf, qst, 1)
    split_queries(qbuf, qst, 2)
    attend(qst, acc, top, 0, kvo.at[0], 1, 3)
    forward(0, 1)
    attend(qst, acc, top, 1, kvo.at[1], 1, 3)
    qg.far()
    split_queries(qbuf, qst, 3)
    for h in range(2):
        attend(qst, acc, top, h, kvo.at[h], 3, 4)
    for s in range(3):
        for h in range(2):
            if s > 0:
                forward(s, h)
            attend(qst, acc, top, h, kvp.at[s, h].reshape(2 * TB, 2 * VD), 0, 4)
    stats = []
    for h in range(2):
        from_l[h].wait_recv()
        from_r[h].wait_recv()
        attend(qst, acc, top, h, kvf.at[h], 0, 4)
        gather_stats(acc, top, stat, h)
        stats.append(
            [link.start(stat.at[h], got.at[p, h], dev) for p, dev in ((1, yr), (0, yl), (2, yf))]
        )
    red = Reduce4(link, part, land, yl, yr)
    for h in range(2):
        for w in stats[h]:
            w.wait_recv()
        blend(acc, stat, got, lam_ref, part, mine, h)
        red.begin(h)
    for h in range(2):
        red.pass_on(h)
    for h in range(2):
        red.end(h)
        cols = slice(h * VD, (h + 1) * VD)
        mixed = mine[:, cols] + land[0, :, cols].astype(F32) + land[1, :, cols].astype(F32)
        scale = lax.rsqrt(jnp.mean(mixed * mixed, axis=1, keepdims=True) + 1e-6)
        att[:, cols] = (mixed * scale * gain_ref[...]).astype(BF16)

    for t in range(2):
        for s, dx in enumerate((0, -1, 1, 2)):
            nx = (x + dx + 4) % 4
            nc = c if t == 0 else 1 - c
            first = pl.multiple_of((2 * nx + nc) * OWN, 16)
            attr[t * 4 * OWN + s * OWN : t * 4 * OWN + (s + 1) * OWN, :] = att[pl.ds(first, OWN), :]

    xred = Reduce4(link, pxb, land2, xl, xr)
    back(link, xred, px, dsend, drecv, pxb, other, lambda cols: jnp.dot(attr[...], ow_ref[:, cols], preferred_element_type=F32))
    after = res_ref[...].astype(F32) + px[0] + land2[0].astype(F32) + land2[1].astype(F32)
    mix_ref[...] = after
    scale = lax.rsqrt(jnp.mean(after * after, axis=1, keepdims=True) + 1e-6)
    rows_ref[0, 0] = (after * scale * ngain_ref[...]).astype(BF16)
    spread(link, rows_ref, xl, xr, other)
    link.finish()


def spread(link, rows, xl, xr, other):
    g = Gather4(link, rows.at[0], xl, xr)
    g.begin()
    waits = [link.start(rows.at[0, 0], rows.at[1, 0], other)]
    g.near()
    waits += [link.start(rows.at[0, s], rows.at[1, s], other) for s in (1, 2)]
    g.far()
    waits.append(link.start(rows.at[0, 3], rows.at[1, 3], other))
    for w in waits:
        w.wait_recv()


def back(link, red, px, dsend, drecv, pxb, other, product):
    step = 512
    sent = []
    for n in range(D // step):
        cols = slice(n * step, (n + 1) * step)
        o = product(cols)
        dsend[n] = o[4 * OWN :].astype(BF16)
        sent.append(link.start(dsend.at[n], drecv.at[n], other))
        px[:, :, cols] = o[: 4 * OWN].reshape(4, OWN, step)
    for n in range(D // step):
        cols = slice(n * step, (n + 1) * step)
        sent[n].wait_recv()
        both = px[:, :, cols] + drecv[n].reshape(4, OWN, step).astype(F32)
        px[0, :, cols] = both[0]
        pxb[1:4, :, cols] = both[1:4].astype(BF16)
        if n % 2 == 1:
            red.begin(n // 2)
    for k in range(2):
        red.pass_on(k)
    for k in range(2):
        red.end(k)


def mixer_kernel(rows_ref, w_ref, mix_ref, out_ref, hid, px, dsend, drecv, pxb, land2, send, recv):
    z, y, x, c, at = places()
    xr, xl, other = at(dx=1), at(dx=-1), at(other=True)
    link = Link(send, recv)
    rows = rows_ref[...]
    for lo in range(0, 640, 128):
        gate = jnp.dot(rows, w_ref[:, lo : lo + 128], preferred_element_type=F32)
        up = jnp.dot(rows, w_ref[:, 640 + lo : 768 + lo], preferred_element_type=F32)
        hid[:, lo : lo + 128] = (gate * jax.nn.sigmoid(gate) * up).astype(BF16)
    tail = jnp.dot(rows, w_ref[:, 1280:1408], preferred_element_type=F32)
    hid[:, 640:] = (tail * jax.nn.sigmoid(tail) * pltpu.roll(tail, 64, 1)).astype(BF16)[:, :64]
    meet((xr, xl, other))
    red = Reduce4(link, pxb, land2, xl, xr)

    def product(cols):
        return lax.dot_general(
            hid[...], w_ref[cols, 2 * FL :], (((1,), (1,)), ((), ())), preferred_element_type=F32
        )

    back(link, red, px, dsend, drecv, pxb, other, product)
    mixer = px[0] + land2[0].astype(F32) + land2[1].astype(F32)
    out_ref[...] = (mix_ref[...] + 0.5 * mixer).astype(BF16)
    link.finish()


def vmem(*shape, dtype=BF16):
    return pltpu.VMEM(shape, dtype)


BACK = [
    vmem(4, OWN, D, dtype=F32),
    vmem(4, 4 * OWN, 512),
    vmem(4, 4 * OWN, 512),
    vmem(4, OWN, D),
    vmem(3, OWN, D),
]


def params(cid):
    return pltpu.CompilerParams(
        collective_id=cid, has_side_effects=True, vmem_limit_bytes=60 * 1024 * 1024
    )


def body(
    residual_in, queries, keys, values, mix_lambda, head_gain, out_weight, norm_gain,
    gate_weight, up_weight, down_weight,
):
    w = jnp.concatenate(
        [gate_weight[:, :640], up_weight[:, :640], gate_weight[:, 640:], up_weight[:, 640:], down_weight.T],
        axis=1,
    )
    w_all = lax.all_gather(w, "sp", axis=0, tiled=True)
    whole = pl.BlockSpec(memory_space=pltpu.VMEM)
    hbm = pl.BlockSpec(memory_space=pl.ANY)
    smem = pl.BlockSpec(memory_space=pltpu.SMEM)
    rows, mix = pl.pallas_call(
        front_kernel,
        out_shape=(
            jax.ShapeDtypeStruct((2, 4, OWN, D), BF16),
            jax.ShapeDtypeStruct((OWN, D), F32),
        ),
        in_specs=[hbm, hbm, hbm, whole, whole, smem, whole, whole],
        out_specs=(whole, whole),
        scratch_shapes=[
            vmem(4, TB, 256),
            vmem(2, 8, TB, VD),
            vmem(2, TB, 256),
            vmem(3, 2, 2, TB, 256),
            vmem(2, TB, 256),
            vmem(2, 8, TB, 256, dtype=F32),
            vmem(2, 8, TB, VD, dtype=F32),
            vmem(2, 64, VD, dtype=F32),
            vmem(3, 2, 64, VD, dtype=F32),
            vmem(4, TB, 256),
            vmem(3, TB, 256),
            vmem(TB, 256, dtype=F32),
            vmem(TB, 256),
            vmem(TB, 256),
            *BACK,
            pltpu.SemaphoreType.DMA((5,)),
            pltpu.SemaphoreType.DMA((64,)),
            pltpu.SemaphoreType.DMA((64,)),
        ],
        compiler_params=params(0),
        name="front",
    )(
        queries, keys, values, residual_in, out_weight, mix_lambda,
        head_gain.reshape(1, VD), norm_gain.reshape(1, D),
    )
    return pl.pallas_call(
        mixer_kernel,
        out_shape=jax.ShapeDtypeStruct((OWN, D), BF16),
        in_specs=[whole, whole, whole],
        out_specs=whole,
        scratch_shapes=[
            vmem(TB, FL),
            *BACK,
            pltpu.SemaphoreType.DMA((16,)),
            pltpu.SemaphoreType.DMA((16,)),
        ],
        compiler_params=params(1),
        name="mixer",
    )(rows.reshape(8 * OWN, D), w_all, mix)


def solution(mesh):
    return jax.shard_map(
        body,
        mesh=mesh,
        in_specs=(
            P(("sp", "tp"), None),
            P("sp", "tp"),
            P("sp", "tp"),
            P("sp", "tp"),
            P("tp"),
            P(),
            P("tp", None),
            P(),
            P("sp", "tp"),
            P("sp", "tp"),
            P("tp", "sp"),
        ),
        out_specs=P(("sp", "tp"), None),
        check_vma=False,
    )
```

```python
import math

import jax
import jax.numpy as jnp
from jax import lax
from jax.experimental import pallas as pl
from jax.experimental.pallas import tpu as pltpu
from jax.sharding import PartitionSpec as P

MESH = pl.DeviceIdType.MESH
F32 = jnp.float32
BF16 = jnp.bfloat16

TB = 384
VD = 128
D = 2048
FL = 704
WC = 3 * FL
OWN = 48
SCALE = math.log2(math.e) / 8.0


class Link:
    def __init__(self, send, recv):
        self.send, self.recv, self.count, self.live = send, recv, 0, []

    def copy(self, src, dst, dev):
        k = self.count
        self.count += 1
        return pltpu.make_async_remote_copy(
            src_ref=src,
            dst_ref=dst,
            send_sem=self.send.at[k],
            recv_sem=self.recv.at[k],
            device_id=dev,
            device_id_type=MESH,
        )

    def start(self, src, dst, dev):
        c = self.copy(src, dst, dev)
        c.start()
        self.live.append(c)
        return c

    def finish(self):
        for c in self.live:
            c.wait_send()


def places():
    sp, tp = lax.axis_index("sp"), lax.axis_index("tp")
    z, y = sp // 4, sp % 4
    x, c = tp // 2, tp % 2

    def at(dz=0, dy=0, dx=0, other=False):
        nz, ny, nx = (z + dz + 8) % 8, (y + dy + 4) % 4, (x + dx + 4) % 4
        nc = 1 - c if other else c
        return (nz * 4 + ny, nx * 2 + nc)

    return z, y, x, c, at


def half(ref, k, axis=1):
    w = ref.shape[axis] // 2
    return ref.at[:, pl.ds(k * w, w)] if axis == 1 else ref.at[pl.ds(k * w, w)]


class Gather4:
    def __init__(self, link, buf, left, right):
        self.link, self.buf, self.left, self.right = link, buf, left, right

    def begin(self):
        b = self.buf
        self.r1 = self.link.start(b.at[0], b.at[1], self.right)
        self.l1 = self.link.start(b.at[0], b.at[2], self.left)

    def near(self):
        b = self.buf
        self.r1.wait_recv()
        self.r2 = self.link.start(half(b.at[1], 0), half(b.at[3], 0), self.right)
        self.l1.wait_recv()
        self.l2 = self.link.start(half(b.at[2], 1), half(b.at[3], 1), self.left)

    def far(self):
        self.r2.wait_recv()
        self.l2.wait_recv()


class Reduce4:
    def __init__(self, link, part, land, left, right, axis):
        self.link, self.part, self.land, self.left, self.right = link, part, land, left, right
        self.axis = axis
        self.far, self.direct, self.sum = [None] * 2, [None] * 2, [None] * 2

    def cut(self, ref, slot, k):
        return half(ref.at[slot], k, self.axis)

    def begin(self, k):
        p, t = self.part, self.land
        dev, near = (self.right, self.left) if k == 0 else (self.left, self.right)
        self.far[k] = self.link.start(self.cut(p, 3, k), self.cut(t, 2, k), dev)
        slot, to = (1, 1) if k == 0 else (2, 0)
        self.direct[k] = self.link.start(self.cut(p, slot, k), self.cut(t, to, k), near)

    def pass_on(self, k):
        p, t = self.part, self.land
        self.far[k].wait_recv()
        slot = 2 if k == 0 else 1
        w = p.shape[1 + self.axis] // 2
        cut = slice(k * w, (k + 1) * w)
        at = (slot, cut) if self.axis == 0 else (slot, slice(None), cut)
        way = (2, *at[1:])
        p[at] = (p[at].astype(F32) + t[way].astype(F32)).astype(BF16)
        to, dev = (0, self.right) if k == 0 else (1, self.left)
        self.sum[k] = self.link.start(self.cut(p, slot, k), self.cut(t, to, k), dev)

    def end(self, k):
        self.direct[k].wait_recv()
        self.sum[k].wait_recv()


def attend(qst, acc, top, h, keys, slots):
    n = keys.shape[0]
    kk = keys[:, :VD]
    vt = jnp.concatenate(
        [keys[VD * j : VD * (j + 1), VD:] for j in range(n // VD)], axis=1
    )
    vt = jnp.concatenate([vt, jnp.ones((16, n), BF16)], axis=0)

    def scores(t):
        return lax.dot_general(kk, qst[h, t], (((1,), (1,)), ((), ())), preferred_element_type=F32)

    def weigh(t, s):
        old = top[h, t]
        new = jnp.maximum(old, jnp.max(s, axis=0, keepdims=True))
        alpha = jnp.exp2((old - new) * SCALE)
        top[h, t] = new
        return jnp.exp2((s - new[:1]) * SCALE).astype(BF16), alpha

    def add(t, p, alpha):
        acc[h, t] = acc[h, t] * alpha[:1] + jnp.dot(vt, p, preferred_element_type=F32)

    s, before = scores(slots[0]), None
    for j, t in enumerate(slots):
        following = scores(slots[j + 1]) if j + 1 < len(slots) else None
        p, alpha = weigh(t, s)
        if before is not None:
            add(*before)
        before, s = (t, p, alpha), following
    add(*before)


def split_queries(qbuf, qst, slot):
    lane = lax.broadcasted_iota(jnp.int32, (TB, VD), 1)
    for h in range(2):
        q = qbuf[slot, :, h * VD : (h + 1) * VD]
        zero = jnp.zeros_like(q)
        qst[h, slot, :TB, :] = jnp.where(lane < 64, q, zero)
        qst[h, slot, TB:, :] = jnp.where(lane < 64, zero, q)


SLOTS = ((1, 3, 0, 2), (2, 0, 3, 1), (3, 2, 1, 0))


def blend(acc, stat, got, lam, part, mine, h):
    def peer(p, base):
        return jnp.concatenate([got[p, h, base + s : base + s + 1, :] for s in SLOTS[p]], axis=0)

    tops = [stat[h, :4, :]] + [peer(p, 0) for p in range(3)]
    sums = [stat[h, 4:, :]] + [peer(p, 4) for p in range(3)]
    top = jnp.maximum(jnp.maximum(tops[0], tops[1]), jnp.maximum(tops[2], tops[3]))
    weights = [jnp.exp2((t - top) * SCALE) for t in tops]
    total = sum(w * s for w, s in zip(weights, sums))
    lane = lax.broadcasted_iota(jnp.int32, (4, 2 * TB), 1)
    factor = jnp.where(lane < TB, 1.0, -lam[h]) * weights[0] / total
    rows = slice(h * VD, (h + 1) * VD)
    for s in (3, 1, 2, 0):
        m = (
            acc[h, s, :VD, :TB] * factor[s : s + 1, :TB]
            + acc[h, s, :VD, TB:] * factor[s : s + 1, TB:]
        )
        if s == 0:
            mine[rows, :] = m
        else:
            part[s, rows, :] = m.astype(BF16)


def layer_kernel(
    q_hbm, k_hbm, v_hbm, res_hbm, ow_hbm, gate_hbm, up_hbm, down_hbm, lam_ref, gain_ref, ngain_ref,
    out_ref,
    qbuf, qst, kvo, kvp, kvf, acc, top, stat, got, part, land, mine,
    att, attr, rows, after, wa, wb, vin, gin, uin, ow, res, hid,
    px, dsend, drecv, pxb, land2, dsend2, drecv2, pxb2, land3, lsem, send, recv,
):
    z, y, x, c, at = places()
    zr, zl, yr, yl, yf = at(dz=1), at(dz=-1), at(dy=1), at(dy=-1), at(dy=2)
    xr, xl, other = at(dx=1), at(dx=-1), at(other=True)
    loads = []

    def load(src, dst):
        l = pltpu.make_async_copy(src, dst, lsem.at[len(loads)])
        l.start()
        loads.append(l)
        return l

    def block(dz, dy):
        return pl.ds(pl.multiple_of((((z + dz + 8) % 8) * 4 + (y + dy + 4) % 4) * 64, 64), 64)

    def plane(dz):
        return pl.ds(pl.multiple_of(((z + dz + 8) % 8) * 256, 256), 256)

    first = [load(v_hbm, vin), load(q_hbm, qbuf.at[0])]
    for h in range(2):
        first.append(load(k_hbm.at[:, pl.ds(h * VD, VD)], kvo.at[h, :, pl.ds(0, VD)]))
    second = [load(gate_hbm, gin), load(up_hbm, uin), load(down_hbm, wb.at[block(0, 0)])]
    third = [load(ow_hbm, ow), load(res_hbm, res)]
    link = Link(send, recv)
    barrier = pltpu.get_barrier_semaphore()
    peers = (zr, zl, yr, yl, yf, xr, xl, other)
    for dev in peers:
        pl.semaphore_signal(barrier, inc=1, device_id=dev, device_id_type=MESH)
    acc[...] = jnp.zeros_like(acc)
    top[...] = jnp.full_like(top, -1e30)
    for l in first:
        l.wait()
    for h in range(2):
        for j in range(3):
            r = slice(j * VD, (j + 1) * VD)
            kvo[h, r, VD:] = jnp.transpose(vin[r, h * VD : (h + 1) * VD])
    for l in second:
        l.wait()
    mine_rows = block(0, 0)
    for j in range(5):
        cols = slice(j * VD, (j + 1) * VD)
        wa[mine_rows, 2 * j * VD : (2 * j + 1) * VD] = gin[:, cols]
        wa[mine_rows, (2 * j + 1) * VD : (2 * j + 2) * VD] = uin[:, cols]
    wa[mine_rows, 10 * VD :] = jnp.concatenate([gin[:, 640:], uin[:, 640:]], axis=1)
    pl.semaphore_wait(barrier, len(peers))

    qg = Gather4(link, qbuf, yl, yr)
    qg.begin()
    from_l, from_r = [None, None], [None, None]
    for h in range(2):
        from_l[h] = link.start(kvo.at[h], kvp.at[0, h, 0], zr)
        from_r[h] = link.start(kvo.at[h], kvp.at[0, h, 1], zl)

    def forward(s, h):
        from_l[h].wait_recv()
        if s < 2:
            nl = link.start(kvp.at[s, h, 0], kvp.at[s + 1, h, 0], zr)
        else:
            nl = link.start(kvp.at[s, h, 0, pl.ds(0, TB // 2)], kvf.at[h, pl.ds(0, TB // 2)], zr)
        from_r[h].wait_recv()
        if s < 2:
            nr = link.start(kvp.at[s, h, 1], kvp.at[s + 1, h, 1], zl)
        else:
            nr = link.start(kvp.at[s, h, 1, pl.ds(TB // 2, TB // 2)], kvf.at[h, pl.ds(TB // 2, TB // 2)], zl)
        from_l[h], from_r[h] = nl, nr

    wz, wy, ends = {}, {}, []

    def a_along_z(s):
        rl, rr = block(-s, 0), block(s, 0)
        if s > 0:
            wz[s][0].wait_recv()
            wz[s][1].wait_recv()
        if s < 3:
            wz[s + 1] = (
                link.start(wa.at[rl], wa.at[rl], zr),
                link.start(wa.at[rr], wa.at[rr], zl),
            )
        else:
            lo, hi = pl.ds(0, 640), pl.ds(640, 768)
            wz[4] = (
                link.start(wa.at[rl, lo], wa.at[rl, lo], zr),
                link.start(wa.at[rr, hi], wa.at[rr, hi], zl),
            )

    def a_start_y(dz):
        b = block(dz, 0)
        wy[dz] = (link.start(wa.at[b], wa.at[b], yr), link.start(wa.at[b], wa.at[b], yl))

    def a_middle_y(dz):
        wy[dz][0].wait_recv()
        bl, br = block(dz, -1), block(dz, 1)
        lo, hi = pl.ds(0, 640), pl.ds(640, 768)
        ends.append(link.start(wa.at[bl, lo], wa.at[bl, lo], yr))
        wy[dz][1].wait_recv()
        ends.append(link.start(wa.at[br, hi], wa.at[br, hi], yl))

    bq = []

    def b_start_y():
        b = block(0, 0)
        bq.extend([link.start(wb.at[b], wb.at[b], yr), link.start(wb.at[b], wb.at[b], yl)])

    def b_middle_y():
        bl, br = block(0, -1), block(0, 1)
        lo, hi = pl.ds(0, 384), pl.ds(384, 320)
        bq[0].wait_recv()
        bq.append(link.start(wb.at[bl, lo], wb.at[bl, lo], yr))
        bq[1].wait_recv()
        bq.append(link.start(wb.at[br, hi], wb.at[br, hi], yl))

    bz = {}

    def b_along_z(s):
        if s == 0:
            bq[2].wait_recv()
            bq[3].wait_recv()
        else:
            bz[s][0].wait_recv()
            bz[s][1].wait_recv()
        rl, rr = plane(-s), plane(s)
        if s == 3:
            base = ((z + 5) % 8) * 256, ((z + 3) % 8) * 256
            rl = pl.ds(pl.multiple_of(base[0], 128), 128)
            rr = pl.ds(pl.multiple_of(base[1] + 128, 128), 128)
        bz[s + 1] = (
            link.start(wb.at[rl], wb.at[rl], zr),
            link.start(wb.at[rr], wb.at[rr], zl),
        )

    a_along_z(0)
    a_start_y(0)
    b_start_y()
    split_queries(qbuf, qst, 0)
    for h in range(2):
        attend(qst, acc, top, h, kvo.at[h], (0,))
    qg.near()
    forward(0, 0)
    split_queries(qbuf, qst, 1)
    split_queries(qbuf, qst, 2)
    attend(qst, acc, top, 0, kvo.at[0], (1, 2))
    forward(0, 1)
    attend(qst, acc, top, 1, kvo.at[1], (1, 2))
    qg.far()
    split_queries(qbuf, qst, 3)
    for h in range(2):
        attend(qst, acc, top, h, kvo.at[h], (3,))

    def pair(s, h):
        attend(qst, acc, top, h, kvp.at[s, h].reshape(2 * TB, 2 * VD), (0, 1, 2, 3))

    a_middle_y(0)
    b_middle_y()
    pair(0, 0)
    forward(1, 0)
    pair(0, 1)
    forward(1, 1)
    a_along_z(1)
    a_start_y(-1)
    a_start_y(1)
    pair(1, 0)
    forward(2, 0)
    pair(1, 1)
    forward(2, 1)
    pair(2, 0)
    a_middle_y(-1)
    a_middle_y(1)
    pair(2, 1)
    a_along_z(2)
    stats = []
    for h in range(2):
        from_l[h].wait_recv()
        from_r[h].wait_recv()
        attend(qst, acc, top, h, kvf.at[h], (0, 1, 2, 3))
        stat[h] = jnp.concatenate(
            [top[h, s, :1, :] for s in range(4)] + [acc[h, s, VD : VD + 1, :] for s in range(4)],
            axis=0,
        )
        stats.append(
            [link.start(stat.at[h], got.at[p, h], dev) for p, dev in ((1, yr), (0, yl), (2, yf))]
        )
    b_along_z(0)
    red = Reduce4(link, part, land, yl, yr, 0)
    for h in range(2):
        for w in stats[h]:
            w.wait_recv()
        blend(acc, stat, got, lam_ref, part, mine, h)
        red.begin(h)
    for h in range(2):
        red.pass_on(h)
    a_start_y(-2)
    a_start_y(2)
    a_along_z(3)
    a_start_y(-3)
    a_start_y(3)
    for l in third:
        l.wait()
    for h in range(2):
        red.end(h)
        r = slice(h * VD, (h + 1) * VD)
        mixed = mine[r, :] + land[0, r, :].astype(F32) + land[1, r, :].astype(F32)
        scale = lax.rsqrt(jnp.mean(mixed * mixed, axis=0, keepdims=True) + 1e-6)
        att[:, r] = jnp.transpose(mixed * scale * gain_ref[...]).astype(BF16)

    for t in range(2):
        for s, dx in enumerate((0, -1, 1, 2)):
            nx = (x + dx + 4) % 4
            nc = c if t == 0 else 1 - c
            begin = pl.multiple_of((2 * nx + nc) * OWN, 16)
            attr[t * 4 * OWN + s * OWN : t * 4 * OWN + (s + 1) * OWN, :] = att[pl.ds(begin, OWN), :]

    def project(cols):
        return jnp.dot(attr[...], ow[:, cols], preferred_element_type=F32)

    def between():
        b_along_z(1)
        a_middle_y(-2)
        a_middle_y(2)

    back(link, Reduce4(link, pxb, land2, xl, xr, 1), px, dsend, drecv, pxb, other, project, between)
    total = res[...].astype(F32) + px[0] + land2[0].astype(F32) + land2[1].astype(F32)
    after[...] = total
    scale = lax.rsqrt(jnp.mean(total * total, axis=1, keepdims=True) + 1e-6)
    rows[0, 0] = (total * scale * ngain_ref[...]).astype(BF16)

    def later():
        a_middle_y(-3)
        a_middle_y(3)
        wz[4][0].wait_recv()
        wz[4][1].wait_recv()
        a_start_y(4)
        b_along_z(2)

    spread(link, rows, xl, xr, other, later)
    b_along_z(3)
    a_middle_y(4)
    for e in ends:
        e.wait_recv()
    flat = rows[...].reshape(8 * OWN, D)
    for j in range(6):
        w = 2 * VD if j < 5 else VD
        both = jnp.dot(flat, wa[:, 2 * VD * j : 2 * VD * j + w], preferred_element_type=F32)
        gate = both[:, :VD]
        if j < 5:
            hid[:, j * VD : (j + 1) * VD] = (gate * jax.nn.sigmoid(gate) * both[:, VD:]).astype(BF16)
        else:
            last = gate * jax.nn.sigmoid(gate) * pltpu.roll(gate, 64, 1)
            hid[:, 5 * VD :] = last.astype(BF16)[:, :64]
    bz[4][0].wait_recv()
    bz[4][1].wait_recv()

    def down(cols):
        return lax.dot_general(
            hid[...], wb[cols, :], (((1,), (1,)), ((), ())), preferred_element_type=F32
        )

    back(link, Reduce4(link, pxb2, land3, xl, xr, 1), px, dsend2, drecv2, pxb2, other, down, None)
    mixer = px[0] + land3[0].astype(F32) + land3[1].astype(F32)
    out_ref[...] = (after[...] + 0.5 * mixer).astype(BF16)
    link.finish()


def spread(link, rows, xl, xr, other, later):
    g = Gather4(link, rows.at[0], xl, xr)
    g.begin()
    waits = [link.start(rows.at[0, 0], rows.at[1, 0], other)]
    g.near()
    waits += [link.start(rows.at[0, s], rows.at[1, s], other) for s in (1, 2)]
    later()
    g.far()
    waits.append(link.start(rows.at[0, 3], rows.at[1, 3], other))
    for w in waits:
        w.wait_recv()


def back(link, red, px, dsend, drecv, pxb, other, product, between):
    step = 512
    sent = []
    for n in range(D // step):
        cols = slice(n * step, (n + 1) * step)
        o = product(cols)
        dsend[n] = o[4 * OWN :].astype(BF16)
        sent.append(link.start(dsend.at[n], drecv.at[n], other))
        px[:, :, cols] = o[: 4 * OWN].reshape(4, OWN, step)
    for n in range(D // step):
        cols = slice(n * step, (n + 1) * step)
        sent[n].wait_recv()
        both = px[:, :, cols] + drecv[n].reshape(4, OWN, step).astype(F32)
        px[0, :, cols] = both[0]
        pxb[1:4, :, cols] = both[1:4].astype(BF16)
        if n % 2 == 1:
            red.begin(n // 2)
    if between is not None:
        between()
    for k in range(2):
        red.pass_on(k)
    for k in range(2):
        red.end(k)


def vmem(*shape, dtype=BF16):
    return pltpu.VMEM(shape, dtype)


BACK = [
    vmem(4, 4 * OWN, 512),
    vmem(4, 4 * OWN, 512),
    vmem(4, OWN, D),
    vmem(3, OWN, D),
]


def params(cid):
    return pltpu.CompilerParams(
        collective_id=cid, has_side_effects=True, vmem_limit_bytes=60 * 1024 * 1024
    )


def body(
    residual_in, queries, keys, values, mix_lambda, head_gain, out_weight, norm_gain,
    gate_weight, up_weight, down_weight,
):
    whole = pl.BlockSpec(memory_space=pltpu.VMEM)
    hbm = pl.BlockSpec(memory_space=pl.ANY)
    smem = pl.BlockSpec(memory_space=pltpu.SMEM)
    return pl.pallas_call(
        layer_kernel,
        out_shape=jax.ShapeDtypeStruct((OWN, D), BF16),
        in_specs=[hbm] * 8 + [smem, whole, whole],
        out_specs=whole,
        scratch_shapes=[
            vmem(4, TB, 256),
            vmem(2, 4, 2 * TB, VD),
            vmem(2, TB, 256),
            vmem(3, 2, 2, TB, 256),
            vmem(2, TB, 256),
            vmem(2, 4, VD + 16, 2 * TB, dtype=F32),
            vmem(2, 4, 8, 2 * TB, dtype=F32),
            vmem(2, 8, 2 * TB, dtype=F32),
            vmem(3, 2, 8, 2 * TB, dtype=F32),
            vmem(4, 256, TB),
            vmem(3, 256, TB),
            vmem(256, TB, dtype=F32),
            vmem(TB, 256),
            vmem(TB, 256),
            vmem(2, 4, OWN, D),
            vmem(OWN, D, dtype=F32),
            vmem(D, 2 * FL),
            vmem(D, FL),
            vmem(TB, 256),
            vmem(64, FL),
            vmem(64, FL),
            vmem(256, D),
            vmem(OWN, D),
            vmem(TB, FL),
            vmem(4, OWN, D, dtype=F32),
            *BACK,
            *BACK,
            pltpu.SemaphoreType.DMA((9,)),
            pltpu.SemaphoreType.DMA((160,)),
            pltpu.SemaphoreType.DMA((160,)),
        ],
        compiler_params=params(0),
        name="layer",
    )(
        queries, keys, values, residual_in, out_weight, gate_weight, up_weight, down_weight.T,
        mix_lambda, head_gain.reshape(VD, 1), norm_gain.reshape(1, D),
    )


def solution(mesh):
    return jax.shard_map(
        body,
        mesh=mesh,
        in_specs=(
            P(("sp", "tp"), None),
            P("sp", "tp"),
            P("sp", "tp"),
            P("sp", "tp"),
            P("tp"),
            P(),
            P("tp", None),
            P(),
            P("sp", "tp"),
            P("sp", "tp"),
            P("tp", "sp"),
        ),
        out_specs=P(("sp", "tp"), None),
        check_vma=False,
    )
```

```python
import math

import jax
import jax.numpy as jnp
from jax import lax
from jax.experimental import pallas as pl
from jax.experimental.pallas import tpu as pltpu
from jax.sharding import PartitionSpec as P

MESH = pl.DeviceIdType.MESH
F32 = jnp.float32
BF16 = jnp.bfloat16

TB = 384
VD = 128
D = 2048
FL = 704
WC = 3 * FL
OWN = 48
SCALE = math.log2(math.e) / 8.0


class Link:
    def __init__(self, send, recv):
        self.send, self.recv, self.count, self.live = send, recv, 0, []

    def copy(self, src, dst, dev):
        k = self.count
        self.count += 1
        return pltpu.make_async_remote_copy(
            src_ref=src,
            dst_ref=dst,
            send_sem=self.send.at[k],
            recv_sem=self.recv.at[k],
            device_id=dev,
            device_id_type=MESH,
        )

    def start(self, src, dst, dev):
        c = self.copy(src, dst, dev)
        c.start()
        self.live.append(c)
        return c

    def finish(self, count=None):
        done = self.live[:count]
        self.live = self.live[len(done) :]
        for c in done:
            c.wait_send()


def places():
    sp, tp = lax.axis_index("sp"), lax.axis_index("tp")
    z, y = sp // 4, sp % 4
    x, c = tp // 2, tp % 2

    def at(dz=0, dy=0, dx=0, other=False):
        nz, ny, nx = (z + dz + 8) % 8, (y + dy + 4) % 4, (x + dx + 4) % 4
        nc = 1 - c if other else c
        return (nz * 4 + ny, nx * 2 + nc)

    return z, y, x, c, at


def half(ref, k, axis=1):
    w = ref.shape[axis] // 2
    return ref.at[:, pl.ds(k * w, w)] if axis == 1 else ref.at[pl.ds(k * w, w)]


class Gather4:
    def __init__(self, link, buf, left, right):
        self.link, self.buf, self.left, self.right = link, buf, left, right

    def begin(self):
        b = self.buf
        self.r, self.l = [None] * 2, [None] * 2
        for k in range(2):
            self.r[k] = self.link.start(half(b.at[0], k), half(b.at[1], k), self.right)
            self.l[1 - k] = self.link.start(half(b.at[0], 1 - k), half(b.at[2], 1 - k), self.left)

    def near(self):
        b = self.buf
        self.r[0].wait_recv()
        self.r2 = self.link.start(half(b.at[1], 0), half(b.at[3], 0), self.right)
        self.l[1].wait_recv()
        self.l2 = self.link.start(half(b.at[2], 1), half(b.at[3], 1), self.left)

    def rest(self):
        self.r[1].wait_recv()
        self.l[0].wait_recv()

    def far(self):
        self.r2.wait_recv()
        self.l2.wait_recv()


class Reduce4:
    def __init__(self, link, part, land, left, right, axis):
        self.link, self.part, self.land, self.left, self.right = link, part, land, left, right
        self.axis = axis
        self.far, self.direct, self.sum = [None] * 2, [None] * 2, [None] * 2

    def cut(self, ref, slot, k):
        return half(ref.at[slot], k, self.axis)

    def begin(self, k):
        p, t = self.part, self.land
        dev = self.right if k == 0 else self.left
        self.far[k] = self.link.start(self.cut(p, 3, k), self.cut(t, 2, k), dev)

    def rest(self, k):
        p, t, near = self.part, self.land, self.left if k == 0 else self.right
        slot, to = (1, 1) if k == 0 else (2, 0)
        self.direct[k] = self.link.start(self.cut(p, slot, k), self.cut(t, to, k), near)

    def pass_on(self, k):
        p, t = self.part, self.land
        self.far[k].wait_recv()
        slot = 2 if k == 0 else 1
        w = p.shape[1 + self.axis] // 2
        cut = slice(k * w, (k + 1) * w)
        at = (slot, cut) if self.axis == 0 else (slot, slice(None), cut)
        way = (2, *at[1:])
        p[at] = (p[at].astype(F32) + t[way].astype(F32)).astype(BF16)
        to, dev = (0, self.right) if k == 0 else (1, self.left)
        self.sum[k] = self.link.start(self.cut(p, slot, k), self.cut(t, to, k), dev)

    def end(self, k):
        self.direct[k].wait_recv()
        self.sum[k].wait_recv()


def attend(qst, acc, top, h, keys, slots):
    n = keys.shape[0]
    kk = keys[:, :VD]
    vt = jnp.concatenate(
        [keys[VD * j : VD * (j + 1), VD:] for j in range(n // VD)], axis=1
    )
    vt = jnp.concatenate([vt, jnp.ones((16, n), BF16)], axis=0)

    def scores(t):
        return lax.dot_general(kk, qst[h, t], (((1,), (1,)), ((), ())), preferred_element_type=F32)

    def weigh(t, s):
        old = top[h, t]
        new = jnp.maximum(old, jnp.max(s, axis=0, keepdims=True))
        alpha = jnp.exp2((old - new) * SCALE)
        top[h, t] = new
        return jnp.exp2((s - new[:1]) * SCALE).astype(BF16), alpha

    def add(t, p, alpha):
        acc[h, t] = acc[h, t] * alpha[:1] + jnp.dot(vt, p, preferred_element_type=F32)

    s, before = scores(slots[0]), None
    for j, t in enumerate(slots):
        following = scores(slots[j + 1]) if j + 1 < len(slots) else None
        p, alpha = weigh(t, s)
        if before is not None:
            add(*before)
        before, s = (t, p, alpha), following
    add(*before)


def split_queries(qbuf, qst, slot, heads=(0, 1)):
    lane = lax.broadcasted_iota(jnp.int32, (TB, VD), 1)
    for h in heads:
        q = qbuf[slot, :, h * VD : (h + 1) * VD]
        zero = jnp.zeros_like(q)
        qst[h, slot, :TB, :] = jnp.where(lane < 64, q, zero)
        qst[h, slot, TB:, :] = jnp.where(lane < 64, zero, q)


SLOTS = ((1, 3, 0, 2), (2, 0, 3, 1), (3, 2, 1, 0))


def blend(acc, stat, got, lam, part, mine, h):
    def peer(p, base):
        return jnp.concatenate([got[p, h, base + s : base + s + 1, :] for s in SLOTS[p]], axis=0)

    tops = [stat[h, :4, :]] + [peer(p, 0) for p in range(3)]
    sums = [stat[h, 4:, :]] + [peer(p, 4) for p in range(3)]
    top = jnp.maximum(jnp.maximum(tops[0], tops[1]), jnp.maximum(tops[2], tops[3]))
    weights = [jnp.exp2((t - top) * SCALE) for t in tops]
    total = sum(w * s for w, s in zip(weights, sums))
    lane = lax.broadcasted_iota(jnp.int32, (4, 2 * TB), 1)
    factor = jnp.where(lane < TB, 1.0, -lam[h]) * weights[0] / total
    rows = slice(h * VD, (h + 1) * VD)
    for s in (3, 1, 2, 0):
        m = (
            acc[h, s, :VD, :TB] * factor[s : s + 1, :TB]
            + acc[h, s, :VD, TB:] * factor[s : s + 1, TB:]
        )
        if s == 0:
            mine[rows, :] = m
        else:
            part[h, s] = m.astype(BF16)


def layer_kernel(
    q_hbm, k_hbm, v_hbm, res_hbm, ow_hbm, gate_hbm, up_hbm, down_hbm, lam_ref, gain_ref, ngain_ref,
    out_ref,
    qbuf, qst, kvo, kvp, kvf, acc, top, stat, got, part, land, mine,
    att, attr, rows, after, wa, wb, vin, gin, uin, ow, res, hid,
    px, dsend, drecv, pxb, land2, dsend2, drecv2, pxb2, land3, lsem, send, recv,
):
    z, y, x, c, at = places()
    zr, zl, yr, yl, yf = at(dz=1), at(dz=-1), at(dy=1), at(dy=-1), at(dy=2)
    xr, xl, other = at(dx=1), at(dx=-1), at(other=True)
    loads = []

    def load(src, dst):
        l = pltpu.make_async_copy(src, dst, lsem.at[len(loads)])
        l.start()
        loads.append(l)
        return l

    def block(dz, dy):
        return pl.ds(pl.multiple_of((((z + dz + 8) % 8) * 4 + (y + dy + 4) % 4) * 64, 64), 64)

    def plane(dz):
        return pl.ds(pl.multiple_of(((z + dz + 8) % 8) * 256, 256), 256)

    first = [load(v_hbm, vin), load(q_hbm, qbuf.at[0])]
    for h in range(2):
        first.append(load(k_hbm.at[:, pl.ds(h * VD, VD)], kvo.at[h, :, pl.ds(0, VD)]))
    second = [load(gate_hbm, gin), load(up_hbm, uin), load(down_hbm, wb.at[block(0, 0)])]
    third = [load(ow_hbm, ow), load(res_hbm, res)]
    link = Link(send, recv)
    barrier = pltpu.get_barrier_semaphore()
    peers = (zr, zl, yr, yl, yf, xr, xl, other)
    for dev in peers:
        pl.semaphore_signal(barrier, inc=1, device_id=dev, device_id_type=MESH)
    acc[...] = jnp.zeros_like(acc)
    top[...] = jnp.full_like(top, -1e30)
    for l in first:
        l.wait()
    for h in range(2):
        for j in range(3):
            r = slice(j * VD, (j + 1) * VD)
            kvo[h, r, VD:] = jnp.transpose(vin[r, h * VD : (h + 1) * VD])
    for l in second:
        l.wait()
    mine_rows = block(0, 0)
    for j in range(5):
        cols = slice(j * VD, (j + 1) * VD)
        wa[mine_rows, 2 * j * VD : (2 * j + 1) * VD] = gin[:, cols]
        wa[mine_rows, (2 * j + 1) * VD : (2 * j + 2) * VD] = uin[:, cols]
    wa[mine_rows, 10 * VD :] = jnp.concatenate([gin[:, 640:], uin[:, 640:]], axis=1)
    pl.semaphore_wait(barrier, len(peers))

    qg = Gather4(link, qbuf, yl, yr)
    qg.begin()
    b = block(0, 0)
    wz = {1: (link.start(wa.at[b], wa.at[b], zr), link.start(wa.at[b], wa.at[b], zl))}
    from_l, from_r = [None, None], [None, None]
    for h in range(2):
        from_l[h] = link.start(kvo.at[h], kvp.at[0, h, 0], zr)
        from_r[h] = link.start(kvo.at[h], kvp.at[0, h, 1], zl)

    def forward(s, h):
        from_l[h].wait_recv()
        if s < 2:
            nl = link.start(kvp.at[s, h, 0], kvp.at[s + 1, h, 0], zr)
        else:
            nl = link.start(kvp.at[s, h, 0, pl.ds(0, TB // 2)], kvf.at[h, pl.ds(0, TB // 2)], zr)
        from_r[h].wait_recv()
        if s < 2:
            nr = link.start(kvp.at[s, h, 1], kvp.at[s + 1, h, 1], zl)
        else:
            nr = link.start(kvp.at[s, h, 1, pl.ds(TB // 2, TB // 2)], kvf.at[h, pl.ds(TB // 2, TB // 2)], zl)
        from_l[h], from_r[h] = nl, nr

    wy, ends = {}, []

    def a_along_z(s):
        rl, rr = block(-s, 0), block(s, 0)
        if s < 3:
            wz[s + 1] = (
                link.start(wa.at[rl], wa.at[rl], zr),
                link.start(wa.at[rr], wa.at[rr], zl),
            )
        else:
            lo, hi = pl.ds(0, 640), pl.ds(640, 768)
            wz[4] = (
                link.start(wa.at[rl, lo], wa.at[rl, lo], zr),
                link.start(wa.at[rr, hi], wa.at[rr, hi], zl),
            )

    def arrived(s):
        wz[s][0].wait_recv()
        wz[s][1].wait_recv()

    def a_start_y(dz):
        b = block(dz, 0)
        wy[dz] = (link.start(wa.at[b], wa.at[b], yr), link.start(wa.at[b], wa.at[b], yl))

    def a_middle_y(dz):
        wy[dz][0].wait_recv()
        bl, br = block(dz, -1), block(dz, 1)
        lo, hi = pl.ds(0, 640), pl.ds(640, 768)
        ends.append(link.start(wa.at[bl, lo], wa.at[bl, lo], yr))
        wy[dz][1].wait_recv()
        ends.append(link.start(wa.at[br, hi], wa.at[br, hi], yl))

    bq = []

    def b_start_y():
        b = block(0, 0)
        bq.extend([link.start(wb.at[b], wb.at[b], yr), link.start(wb.at[b], wb.at[b], yl)])

    def b_middle_y():
        bl, br = block(0, -1), block(0, 1)
        lo, hi = pl.ds(0, 384), pl.ds(384, 320)
        bq[0].wait_recv()
        bq.append(link.start(wb.at[bl, lo], wb.at[bl, lo], yr))
        bq[1].wait_recv()
        bq.append(link.start(wb.at[br, hi], wb.at[br, hi], yl))

    bz = {}

    def b_along_z(s):
        if s == 0:
            bq[2].wait_recv()
            bq[3].wait_recv()
        else:
            bz[s][0].wait_recv()
            bz[s][1].wait_recv()
        rl, rr = plane(-s), plane(s)
        if s == 3:
            base = ((z + 5) % 8) * 256, ((z + 3) % 8) * 256
            rl = pl.ds(pl.multiple_of(base[0], 128), 128)
            rr = pl.ds(pl.multiple_of(base[1] + 128, 128), 128)
        bz[s + 1] = (
            link.start(wb.at[rl], wb.at[rl], zr),
            link.start(wb.at[rr], wb.at[rr], zl),
        )

    split_queries(qbuf, qst, 0)
    for h in range(2):
        attend(qst, acc, top, h, kvo.at[h], (0,))
    qg.near()
    a_start_y(0)
    b_start_y()
    split_queries(qbuf, qst, 1, (0,))
    split_queries(qbuf, qst, 2, (1,))
    attend(qst, acc, top, 0, kvo.at[0], (1,))
    attend(qst, acc, top, 1, kvo.at[1], (2,))
    qg.rest()
    split_queries(qbuf, qst, 1, (1,))
    split_queries(qbuf, qst, 2, (0,))
    attend(qst, acc, top, 0, kvo.at[0], (2,))
    attend(qst, acc, top, 1, kvo.at[1], (1,))
    qg.far()
    arrived(1)
    a_start_y(-1)
    a_start_y(1)
    split_queries(qbuf, qst, 3)
    attend(qst, acc, top, 0, kvo.at[0], (3,))
    attend(qst, acc, top, 1, kvo.at[1], (3,))
    forward(0, 0)

    def pair(s, h):
        attend(qst, acc, top, h, kvp.at[s, h].reshape(2 * TB, 2 * VD), (0, 1, 2, 3))

    reds = [
        Reduce4(link, part.at[h], land.at[h], yl, yr, 0) for h in range(2)
    ]
    stats = [None, None]

    def last(h):
        from_l[h].wait_recv()
        from_r[h].wait_recv()
        attend(qst, acc, top, h, kvf.at[h], (0, 1, 2, 3))
        stat[h] = jnp.concatenate(
            [top[h, s, :1, :] for s in range(4)] + [acc[h, s, VD : VD + 1, :] for s in range(4)],
            axis=0,
        )
        stats[h] = [
            link.start(stat.at[h], got.at[p, h], dev) for p, dev in ((2, yf), (1, yr), (0, yl))
        ]

    def merge(h):
        for w in stats[h]:
            w.wait_recv()
        blend(acc, stat, got, lam_ref, part, mine, h)
        for k in range(2):
            reds[h].begin(k)
        for k in range(2):
            reds[h].rest(k)

    pair(0, 0)
    forward(0, 1)
    a_middle_y(0)
    b_middle_y()
    pair(0, 1)
    forward(1, 0)
    pair(1, 0)
    forward(1, 1)
    a_along_z(1)
    a_middle_y(-1)
    a_middle_y(1)
    pair(1, 1)
    forward(2, 0)
    pair(2, 0)
    forward(2, 1)
    b_along_z(0)
    pair(2, 1)
    last(0)
    arrived(2)
    a_start_y(-2)
    a_along_z(2)
    last(1)
    early = len(link.live)
    for l in third:
        l.wait()
    gain = jnp.transpose(jnp.broadcast_to(gain_ref[...], (VD, VD)))[:, :1]
    merge(0)
    merge(1)
    for h in range(2):
        for k in range(2):
            reds[h].pass_on(k)
    a_middle_y(-2)
    a_start_y(2)
    b_along_z(1)
    for h in range(2):
        for k in range(2):
            reds[h].end(k)
        r = slice(h * VD, (h + 1) * VD)
        mixed = mine[r, :] + land[h, 0].astype(F32) + land[h, 1].astype(F32)
        scale = lax.rsqrt(jnp.mean(mixed * mixed, axis=0, keepdims=True) + 1e-6)
        att[:, r] = jnp.transpose(mixed * scale * gain).astype(BF16)
    arrived(3)
    a_along_z(3)
    a_start_y(-3)
    a_start_y(3)

    for t in range(2):
        for s, dx in enumerate((0, -1, 1, 2)):
            nx = (x + dx + 4) % 4
            nc = c if t == 0 else 1 - c
            begin = pl.multiple_of((2 * nx + nc) * OWN, 16)
            attr[t * 4 * OWN + s * OWN : t * 4 * OWN + (s + 1) * OWN, :] = att[pl.ds(begin, OWN), :]

    def project(cols):
        return jnp.dot(attr[...], ow[:, cols], preferred_element_type=F32)

    def between():
        b_along_z(2)
        arrived(4)
        a_start_y(4)
        a_middle_y(2)
        a_middle_y(-3)
        link.finish(early)

    back(
        link, Reduce4(link, pxb, land2, xl, xr, 1), px, dsend, drecv, pxb, other, project,
        between,
    )
    total = res[...].astype(F32) + px[0] + land2[0].astype(F32) + land2[1].astype(F32)
    after[...] = total
    scale = lax.rsqrt(jnp.mean(total * total, axis=1, keepdims=True) + 1e-6)
    rows[0, 0] = (total * scale * ngain_ref[...]).astype(BF16)

    def started():
        a_middle_y(3)
        a_middle_y(4)

    def passed():
        b_along_z(3)

    spread(link, rows, xl, xr, other, started, passed)
    for e in ends:
        e.wait_recv()
    flat = rows[...].reshape(8 * OWN, D)
    for j in range(6):
        w = 2 * VD if j < 5 else VD
        both = jnp.dot(flat, wa[:, 2 * VD * j : 2 * VD * j + w], preferred_element_type=F32)
        gate = both[:, :VD]
        if j < 5:
            hid[:, j * VD : (j + 1) * VD] = (gate * jax.nn.sigmoid(gate) * both[:, VD:]).astype(BF16)
        else:
            last = gate * jax.nn.sigmoid(gate) * pltpu.roll(gate, 64, 1)
            hid[:, 5 * VD :] = last.astype(BF16)[:, :64]
    bz[4][0].wait_recv()
    bz[4][1].wait_recv()

    def down(cols):
        return lax.dot_general(
            hid[...], wb[cols, :], (((1,), (1,)), ((), ())), preferred_element_type=F32
        )

    back(link, Reduce4(link, pxb2, land3, xl, xr, 1), px, dsend2, drecv2, pxb2, other, down, link.finish)
    mixer = px[0] + land3[0].astype(F32) + land3[1].astype(F32)
    out_ref[...] = (after[...] + 0.5 * mixer).astype(BF16)
    link.finish()


def spread(link, rows, xl, xr, other, started, passed):
    g = Gather4(link, rows.at[0], xl, xr)
    g.begin()
    waits = [link.start(rows.at[0, 0], rows.at[1, 0], other)]
    started()
    g.near()
    passed()
    g.rest()
    waits += [link.start(rows.at[0, s], rows.at[1, s], other) for s in (1, 2)]
    g.far()
    waits.append(link.start(rows.at[0, 3], rows.at[1, 3], other))
    for w in waits:
        w.wait_recv()


def back(link, red, px, dsend, drecv, pxb, other, product, between):
    step = 512
    sent = []
    for n in range(D // step):
        cols = slice(n * step, (n + 1) * step)
        o = product(cols)
        dsend[n] = o[4 * OWN :].astype(BF16)
        sent.append(link.start(dsend.at[n], drecv.at[n], other))
        px[:, :, cols] = o[: 4 * OWN].reshape(4, OWN, step)
    for n in range(D // step):
        cols = slice(n * step, (n + 1) * step)
        sent[n].wait_recv()
        both = px[:, :, cols] + drecv[n].reshape(4, OWN, step).astype(F32)
        px[0, :, cols] = both[0]
        pxb[1:4, :, cols] = both[1:4].astype(BF16)
        if n % 2 == 1:
            red.begin(n // 2)
    for k in range(2):
        red.rest(k)
    for k in range(2):
        red.pass_on(k)
    between()
    for k in range(2):
        red.end(k)


def vmem(*shape, dtype=BF16):
    return pltpu.VMEM(shape, dtype)


BACK = [
    vmem(4, 4 * OWN, 512),
    vmem(4, 4 * OWN, 512),
    vmem(4, OWN, D),
    vmem(3, OWN, D),
]


def params(cid):
    return pltpu.CompilerParams(
        collective_id=cid, has_side_effects=True, vmem_limit_bytes=60 * 1024 * 1024
    )


def body(
    residual_in, queries, keys, values, mix_lambda, head_gain, out_weight, norm_gain,
    gate_weight, up_weight, down_weight,
):
    whole = pl.BlockSpec(memory_space=pltpu.VMEM)
    hbm = pl.BlockSpec(memory_space=pl.ANY)
    smem = pl.BlockSpec(memory_space=pltpu.SMEM)
    return pl.pallas_call(
        layer_kernel,
        out_shape=jax.ShapeDtypeStruct((OWN, D), BF16),
        in_specs=[hbm] * 8 + [smem, whole, whole],
        out_specs=whole,
        scratch_shapes=[
            vmem(4, TB, 256),
            vmem(2, 4, 2 * TB, VD),
            vmem(2, TB, 256),
            vmem(3, 2, 2, TB, 256),
            vmem(2, TB, 256),
            vmem(2, 4, VD + 16, 2 * TB, dtype=F32),
            vmem(2, 4, 8, 2 * TB, dtype=F32),
            vmem(2, 8, 2 * TB, dtype=F32),
            vmem(3, 2, 8, 2 * TB, dtype=F32),
            vmem(2, 4, VD, TB),
            vmem(2, 3, VD, TB),
            vmem(256, TB, dtype=F32),
            vmem(TB, 256),
            vmem(TB, 256),
            vmem(2, 4, OWN, D),
            vmem(OWN, D, dtype=F32),
            vmem(D, 2 * FL),
            vmem(D, FL),
            vmem(TB, 256),
            vmem(64, FL),
            vmem(64, FL),
            vmem(256, D),
            vmem(OWN, D),
            vmem(TB, FL),
            vmem(4, OWN, D, dtype=F32),
            *BACK,
            *BACK,
            pltpu.SemaphoreType.DMA((9,)),
            pltpu.SemaphoreType.DMA((160,)),
            pltpu.SemaphoreType.DMA((160,)),
        ],
        compiler_params=params(0),
        name="layer",
    )(
        queries, keys, values, residual_in, out_weight, gate_weight, up_weight, down_weight.T,
        mix_lambda, head_gain.reshape(1, VD), norm_gain.reshape(1, D),
    )


def solution(mesh):
    return jax.shard_map(
        body,
        mesh=mesh,
        in_specs=(
            P(("sp", "tp"), None),
            P("sp", "tp"),
            P("sp", "tp"),
            P("sp", "tp"),
            P("tp"),
            P(),
            P("tp", None),
            P(),
            P("sp", "tp"),
            P("sp", "tp"),
            P("tp", "sp"),
        ),
        out_specs=P(("sp", "tp"), None),
        check_vma=False,
    )
```

```python
import math

import jax
import jax.numpy as jnp
from jax import lax
from jax.experimental import pallas as pl
from jax.experimental.pallas import tpu as pltpu
from jax.sharding import PartitionSpec as P

MESH = pl.DeviceIdType.MESH
F32 = jnp.float32
BF16 = jnp.bfloat16

TB = 384
VD = 128
D = 2048
FL = 704
WC = 3 * FL
OWN = 48
SCALE = math.log2(math.e) / 8.0


class Link:
    def __init__(self, send, recv):
        self.send, self.recv, self.count, self.live = send, recv, 0, []

    def copy(self, src, dst, dev):
        k = self.count
        self.count += 1
        return pltpu.make_async_remote_copy(
            src_ref=src,
            dst_ref=dst,
            send_sem=self.send.at[k],
            recv_sem=self.recv.at[k],
            device_id=dev,
            device_id_type=MESH,
        )

    def start(self, src, dst, dev):
        c = self.copy(src, dst, dev)
        c.start()
        self.live.append(c)
        return c

    def finish(self, count=None):
        done = self.live[:count]
        self.live = self.live[len(done) :]
        for c in done:
            c.wait_send()


def places():
    sp, tp = lax.axis_index("sp"), lax.axis_index("tp")
    z, y = sp // 4, sp % 4
    x, c = tp // 2, tp % 2

    def at(dz=0, dy=0, dx=0, other=False):
        nz, ny, nx = (z + dz + 8) % 8, (y + dy + 4) % 4, (x + dx + 4) % 4
        nc = 1 - c if other else c
        return (nz * 4 + ny, nx * 2 + nc)

    return z, y, x, c, at


def half(ref, k, axis=1):
    w = ref.shape[axis] // 2
    return ref.at[:, pl.ds(k * w, w)] if axis == 1 else ref.at[pl.ds(k * w, w)]


class Gather4:
    def __init__(self, link, buf, left, right):
        self.link, self.buf, self.left, self.right = link, buf, left, right

    def begin(self):
        b = self.buf
        self.r, self.l = [None] * 2, [None] * 2
        for k in range(2):
            self.r[k] = self.link.start(half(b.at[0], k), half(b.at[1], k), self.right)
            self.l[1 - k] = self.link.start(half(b.at[0], 1 - k), half(b.at[2], 1 - k), self.left)

    def near(self):
        b = self.buf
        self.r[0].wait_recv()
        self.r2 = self.link.start(half(b.at[1], 0), half(b.at[3], 0), self.right)
        self.l[1].wait_recv()
        self.l2 = self.link.start(half(b.at[2], 1), half(b.at[3], 1), self.left)

    def rest(self):
        self.r[1].wait_recv()
        self.l[0].wait_recv()

    def far(self):
        self.r2.wait_recv()
        self.l2.wait_recv()


class Reduce4:
    def __init__(self, link, part, land, left, right, axis):
        self.link, self.part, self.land, self.left, self.right = link, part, land, left, right
        self.axis = axis
        self.far, self.direct, self.sum = [None] * 2, [None] * 2, [None] * 2

    def cut(self, ref, slot, k):
        return half(ref.at[slot], k, self.axis)

    def begin(self, k):
        p, t = self.part, self.land
        dev = self.right if k == 0 else self.left
        self.far[k] = self.link.start(self.cut(p, 3, k), self.cut(t, 2, k), dev)

    def rest(self, k):
        p, t, near = self.part, self.land, self.left if k == 0 else self.right
        slot, to = (1, 1) if k == 0 else (2, 0)
        self.direct[k] = self.link.start(self.cut(p, slot, k), self.cut(t, to, k), near)

    def pass_on(self, k):
        p, t = self.part, self.land
        self.far[k].wait_recv()
        slot = 2 if k == 0 else 1
        w = p.shape[1 + self.axis] // 2
        cut = slice(k * w, (k + 1) * w)
        at = (slot, cut) if self.axis == 0 else (slot, slice(None), cut)
        way = (2, *at[1:])
        p[at] = (p[at].astype(F32) + t[way].astype(F32)).astype(BF16)
        to, dev = (0, self.right) if k == 0 else (1, self.left)
        self.sum[k] = self.link.start(self.cut(p, slot, k), self.cut(t, to, k), dev)

    def end(self, k):
        self.direct[k].wait_recv()
        self.sum[k].wait_recv()


def attend(qst, acc, top, h, keys, slots):
    n = keys.shape[0]
    kk = keys[:, :VD]
    vt = jnp.concatenate(
        [keys[VD * j : VD * (j + 1), VD:] for j in range(n // VD)], axis=1
    )
    vt = jnp.concatenate([vt, jnp.ones((16, n), BF16)], axis=0)

    def scores(t):
        return lax.dot_general(kk, qst[h, t], (((1,), (1,)), ((), ())), preferred_element_type=F32)

    def weigh(t, s):
        old = top[h, t]
        new = jnp.maximum(old, jnp.max(s, axis=0, keepdims=True))
        alpha = jnp.exp2((old - new) * SCALE)
        top[h, t] = new
        return jnp.exp2((s - new[:1]) * SCALE).astype(BF16), alpha

    def add(t, p, alpha):
        acc[h, t] = acc[h, t] * alpha[:1] + jnp.dot(vt, p, preferred_element_type=F32)

    s, before = scores(slots[0]), None
    for j, t in enumerate(slots):
        following = scores(slots[j + 1]) if j + 1 < len(slots) else None
        p, alpha = weigh(t, s)
        if before is not None:
            add(*before)
        before, s = (t, p, alpha), following
    add(*before)


def split_queries(qbuf, qst, slot, heads=(0, 1)):
    lane = lax.broadcasted_iota(jnp.int32, (TB, VD), 1)
    for h in heads:
        q = qbuf[slot, :, h * VD : (h + 1) * VD]
        zero = jnp.zeros_like(q)
        qst[h, slot, :TB, :] = jnp.where(lane < 64, q, zero)
        qst[h, slot, TB:, :] = jnp.where(lane < 64, zero, q)


SLOTS = ((1, 3, 0, 2), (2, 0, 3, 1), (3, 2, 1, 0))


def blend(acc, stat, got, lam, part, mine, h):
    def peer(p, base):
        return jnp.concatenate([got[p, h, base + s : base + s + 1, :] for s in SLOTS[p]], axis=0)

    tops = [stat[h, :4, :]] + [peer(p, 0) for p in range(3)]
    sums = [stat[h, 4:, :]] + [peer(p, 4) for p in range(3)]
    top = jnp.maximum(jnp.maximum(tops[0], tops[1]), jnp.maximum(tops[2], tops[3]))
    weights = [jnp.exp2((t - top) * SCALE) for t in tops]
    total = sum(w * s for w, s in zip(weights, sums))
    lane = lax.broadcasted_iota(jnp.int32, (4, 2 * TB), 1)
    factor = jnp.where(lane < TB, 1.0, -lam[h]) * weights[0] / total
    rows = slice(h * VD, (h + 1) * VD)
    for s in (3, 1, 2, 0):
        m = (
            acc[h, s, :VD, :TB] * factor[s : s + 1, :TB]
            + acc[h, s, :VD, TB:] * factor[s : s + 1, TB:]
        )
        if s == 0:
            mine[rows, :] = m
        else:
            part[h, s] = m.astype(BF16)


def layer_kernel(
    q_hbm, k_hbm, v_hbm, res_hbm, ow_hbm, gate_hbm, up_hbm, down_hbm, lam_ref, gain_ref, ngain_ref,
    out_ref,
    qbuf, qst, kvo, kvp, kvf, acc, top, stat, got, part, land, mine,
    att, attr, rows, after, wa, wb, vin, gin, uin, ow, res, hid,
    px, dsend, drecv, pxb, land2, dsend2, drecv2, pxb2, land3, outv, lsem, send, recv,
):
    z, y, x, c, at = places()
    zr, zl, yr, yl, yf = at(dz=1), at(dz=-1), at(dy=1), at(dy=-1), at(dy=2)
    xr, xl, other = at(dx=1), at(dx=-1), at(other=True)
    loads = []

    def load(src, dst):
        l = pltpu.make_async_copy(src, dst, lsem.at[len(loads)])
        l.start()
        loads.append(l)
        return l

    def block(dz, dy):
        return pl.ds(pl.multiple_of((((z + dz + 8) % 8) * 4 + (y + dy + 4) % 4) * 64, 64), 64)

    def plane(dz):
        return pl.ds(pl.multiple_of(((z + dz + 8) % 8) * 256, 256), 256)

    first = [load(v_hbm, vin), load(q_hbm, qbuf.at[0])]
    for h in range(2):
        first.append(load(k_hbm.at[:, pl.ds(h * VD, VD)], kvo.at[h, :, pl.ds(0, VD)]))
    second = [load(gate_hbm, gin), load(up_hbm, uin), load(down_hbm, wb.at[block(0, 0)])]
    third = [load(ow_hbm, ow), load(res_hbm, res)]
    link = Link(send, recv)
    barrier = pltpu.get_barrier_semaphore()
    peers = (zr, zl, yr, yl, yf, xr, xl, other)
    for dev in peers:
        pl.semaphore_signal(barrier, inc=1, device_id=dev, device_id_type=MESH)
    acc[...] = jnp.zeros_like(acc)
    top[...] = jnp.full_like(top, -1e30)
    for l in first:
        l.wait()
    for h in range(2):
        for j in range(3):
            r = slice(j * VD, (j + 1) * VD)
            kvo[h, r, VD:] = jnp.transpose(vin[r, h * VD : (h + 1) * VD])
    for l in second:
        l.wait()
    mine_rows = block(0, 0)
    for j in range(5):
        cols = slice(j * VD, (j + 1) * VD)
        wa[mine_rows, 2 * j * VD : (2 * j + 1) * VD] = gin[:, cols]
        wa[mine_rows, (2 * j + 1) * VD : (2 * j + 2) * VD] = uin[:, cols]
    wa[mine_rows, 10 * VD :] = jnp.concatenate([gin[:, 640:], uin[:, 640:]], axis=1)
    pl.semaphore_wait(barrier, len(peers))

    qg = Gather4(link, qbuf, yl, yr)
    qg.begin()
    b = block(0, 0)
    wz = {1: (link.start(wa.at[b], wa.at[b], zr), link.start(wa.at[b], wa.at[b], zl))}
    from_l, from_r = [None, None], [None, None]
    for h in range(2):
        from_l[h] = link.start(kvo.at[h], kvp.at[0, h, 0], zr)
        from_r[h] = link.start(kvo.at[h], kvp.at[0, h, 1], zl)

    def forward(s, h):
        from_l[h].wait_recv()
        if s < 2:
            nl = link.start(kvp.at[s, h, 0], kvp.at[s + 1, h, 0], zr)
        else:
            nl = link.start(kvp.at[s, h, 0, pl.ds(0, TB // 2)], kvf.at[h, pl.ds(0, TB // 2)], zr)
        from_r[h].wait_recv()
        if s < 2:
            nr = link.start(kvp.at[s, h, 1], kvp.at[s + 1, h, 1], zl)
        else:
            nr = link.start(kvp.at[s, h, 1, pl.ds(TB // 2, TB // 2)], kvf.at[h, pl.ds(TB // 2, TB // 2)], zl)
        from_l[h], from_r[h] = nl, nr

    wy, ends = {}, []

    def a_along_z(s):
        rl, rr = block(-s, 0), block(s, 0)
        if s < 3:
            wz[s + 1] = (
                link.start(wa.at[rl], wa.at[rl], zr),
                link.start(wa.at[rr], wa.at[rr], zl),
            )
        else:
            lo, hi = pl.ds(0, 640), pl.ds(640, 768)
            wz[4] = (
                link.start(wa.at[rl, lo], wa.at[rl, lo], zr),
                link.start(wa.at[rr, hi], wa.at[rr, hi], zl),
            )

    def arrived(s):
        wz[s][0].wait_recv()
        wz[s][1].wait_recv()

    def a_start_y(dz):
        b = block(dz, 0)
        wy[dz] = (link.start(wa.at[b], wa.at[b], yr), link.start(wa.at[b], wa.at[b], yl))

    def a_middle_y(dz):
        wy[dz][0].wait_recv()
        bl, br = block(dz, -1), block(dz, 1)
        lo, hi = pl.ds(0, 640), pl.ds(640, 768)
        ends.append(link.start(wa.at[bl, lo], wa.at[bl, lo], yr))
        wy[dz][1].wait_recv()
        ends.append(link.start(wa.at[br, hi], wa.at[br, hi], yl))

    bq = []

    def b_start_y():
        b = block(0, 0)
        bq.extend([link.start(wb.at[b], wb.at[b], yr), link.start(wb.at[b], wb.at[b], yl)])

    def b_middle_y():
        bl, br = block(0, -1), block(0, 1)
        lo, hi = pl.ds(0, 384), pl.ds(384, 320)
        bq[0].wait_recv()
        bq.append(link.start(wb.at[bl, lo], wb.at[bl, lo], yr))
        bq[1].wait_recv()
        bq.append(link.start(wb.at[br, hi], wb.at[br, hi], yl))

    bz = {}

    def b_along_z(s):
        if s == 0:
            bq[2].wait_recv()
            bq[3].wait_recv()
        else:
            bz[s][0].wait_recv()
            bz[s][1].wait_recv()
        rl, rr = plane(-s), plane(s)
        if s == 3:
            base = ((z + 5) % 8) * 256, ((z + 3) % 8) * 256
            rl = pl.ds(pl.multiple_of(base[0], 128), 128)
            rr = pl.ds(pl.multiple_of(base[1] + 128, 128), 128)
        bz[s + 1] = (
            link.start(wb.at[rl], wb.at[rl], zr),
            link.start(wb.at[rr], wb.at[rr], zl),
        )

    split_queries(qbuf, qst, 0)
    for h in range(2):
        attend(qst, acc, top, h, kvo.at[h], (0,))
    qg.near()
    a_start_y(0)
    b_start_y()
    split_queries(qbuf, qst, 1, (0,))
    split_queries(qbuf, qst, 2, (1,))
    attend(qst, acc, top, 0, kvo.at[0], (1,))
    attend(qst, acc, top, 1, kvo.at[1], (2,))
    qg.rest()
    split_queries(qbuf, qst, 1, (1,))
    split_queries(qbuf, qst, 2, (0,))
    attend(qst, acc, top, 0, kvo.at[0], (2,))
    attend(qst, acc, top, 1, kvo.at[1], (1,))
    qg.far()
    arrived(1)
    a_start_y(-1)
    a_start_y(1)
    split_queries(qbuf, qst, 3)
    attend(qst, acc, top, 0, kvo.at[0], (3,))
    attend(qst, acc, top, 1, kvo.at[1], (3,))
    forward(0, 0)

    def pair(s, h):
        attend(qst, acc, top, h, kvp.at[s, h].reshape(2 * TB, 2 * VD), (0, 1, 2, 3))

    reds = [
        Reduce4(link, part.at[h], land.at[h], yl, yr, 0) for h in range(2)
    ]
    stats = [None, None]

    def last(h):
        from_l[h].wait_recv()
        from_r[h].wait_recv()
        attend(qst, acc, top, h, kvf.at[h], (0, 1, 2, 3))
        stat[h] = jnp.concatenate(
            [top[h, s, :1, :] for s in range(4)] + [acc[h, s, VD : VD + 1, :] for s in range(4)],
            axis=0,
        )
        stats[h] = [
            link.start(stat.at[h], got.at[p, h], dev) for p, dev in ((2, yf), (1, yr), (0, yl))
        ]

    def merge(h):
        for w in stats[h]:
            w.wait_recv()
        blend(acc, stat, got, lam_ref, part, mine, h)
        for k in range(2):
            reds[h].begin(k)
        for k in range(2):
            reds[h].rest(k)

    pair(0, 0)
    forward(0, 1)
    a_middle_y(0)
    b_middle_y()
    pair(0, 1)
    forward(1, 0)
    pair(1, 0)
    forward(1, 1)
    a_along_z(1)
    a_middle_y(-1)
    a_middle_y(1)
    pair(1, 1)
    forward(2, 0)
    pair(2, 0)
    forward(2, 1)
    b_along_z(0)
    pair(2, 1)
    last(0)
    last(1)
    early = len(link.live)
    arrived(2)
    a_start_y(-2)
    a_along_z(2)
    for l in third:
        l.wait()
    gain = jnp.transpose(jnp.broadcast_to(gain_ref[...], (VD, VD)))[:, :1]
    merge(0)
    merge(1)
    b_along_z(1)
    for h in range(2):
        for k in range(2):
            reds[h].pass_on(k)
    a_middle_y(-2)
    a_start_y(2)
    for h in range(2):
        for k in range(2):
            reds[h].end(k)
        r = slice(h * VD, (h + 1) * VD)
        mixed = mine[r, :] + land[h, 0].astype(F32) + land[h, 1].astype(F32)
        scale = lax.rsqrt(jnp.mean(mixed * mixed, axis=0, keepdims=True) + 1e-6)
        att[:, r] = jnp.transpose(mixed * scale * gain).astype(BF16)
    arrived(3)
    a_along_z(3)
    a_start_y(-3)
    a_start_y(3)

    for t in range(2):
        for s, dx in enumerate((0, -1, 1, 2)):
            nx = (x + dx + 4) % 4
            nc = c if t == 0 else 1 - c
            begin = pl.multiple_of((2 * nx + nc) * OWN, 16)
            attr[t * 4 * OWN + s * OWN : t * 4 * OWN + (s + 1) * OWN, :] = att[pl.ds(begin, OWN), :]

    def project(cols):
        return jnp.dot(attr[...], ow[:, cols], preferred_element_type=F32)

    def between():
        arrived(4)
        a_start_y(4)
        a_middle_y(2)
        a_middle_y(-3)
        link.finish(early)

    back(
        link, Reduce4(link, pxb, land2, xl, xr, 1), px, dsend, drecv, pxb, other, project,
        lambda: b_along_z(2), between,
    )
    total = res[...].astype(F32) + px[0] + land2[0].astype(F32) + land2[1].astype(F32)
    after[...] = total
    scale = lax.rsqrt(jnp.mean(total * total, axis=1, keepdims=True) + 1e-6)
    rows[0, 0] = (total * scale * ngain_ref[...]).astype(BF16)

    def started():
        a_middle_y(3)
        a_middle_y(4)

    def passed():
        b_along_z(3)

    spread(link, rows, xl, xr, other, started, passed)
    for e in ends:
        e.wait_recv()
    flat = rows[...].reshape(8 * OWN, D)
    for j in range(6):
        w = 2 * VD if j < 5 else VD
        both = jnp.dot(flat, wa[:, 2 * VD * j : 2 * VD * j + w], preferred_element_type=F32)
        gate = both[:, :VD]
        if j < 5:
            hid[:, j * VD : (j + 1) * VD] = (gate * jax.nn.sigmoid(gate) * both[:, VD:]).astype(BF16)
        else:
            last = gate * jax.nn.sigmoid(gate) * pltpu.roll(gate, 64, 1)
            hid[:, 5 * VD :] = last.astype(BF16)[:, :64]
    bz[4][0].wait_recv()
    bz[4][1].wait_recv()

    def down(cols):
        return lax.dot_general(
            hid[...], wb[cols, :], (((1,), (1,)), ((), ())), preferred_element_type=F32
        )

    back(link, Reduce4(link, pxb2, land3, xl, xr, 1), px, dsend2, drecv2, pxb2, other, down, lambda: None, link.finish)
    puts = []
    for k in range(2):
        cols = slice(k * D // 2, (k + 1) * D // 2)
        mixer = px[0, :, cols] + land3[0, :, cols].astype(F32) + land3[1, :, cols].astype(F32)
        outv[:, cols] = (after[:, cols] + 0.5 * mixer).astype(BF16)
        puts.append(load(outv.at[:, pl.ds(k * D // 2, D // 2)], out_ref.at[:, pl.ds(k * D // 2, D // 2)]))
    for l in puts:
        l.wait()
    link.finish()


def spread(link, rows, xl, xr, other, started, passed):
    g = Gather4(link, rows.at[0], xl, xr)
    g.begin()
    waits = [link.start(rows.at[0, 0], rows.at[1, 0], other)]
    started()
    g.near()
    passed()
    g.rest()
    waits += [link.start(rows.at[0, s], rows.at[1, s], other) for s in (1, 2)]
    g.far()
    waits.append(link.start(rows.at[0, 3], rows.at[1, 3], other))
    for w in waits:
        w.wait_recv()


def back(link, red, px, dsend, drecv, pxb, other, product, ahead, between):
    step = 512
    sent = []
    for n in range(D // step):
        cols = slice(n * step, (n + 1) * step)
        o = product(cols)
        dsend[n] = o[4 * OWN :].astype(BF16)
        sent.append(link.start(dsend.at[n], drecv.at[n], other))
        px[:, :, cols] = o[: 4 * OWN].reshape(4, OWN, step)
    for n in range(D // step):
        cols = slice(n * step, (n + 1) * step)
        sent[n].wait_recv()
        both = px[:, :, cols] + drecv[n].reshape(4, OWN, step).astype(F32)
        px[0, :, cols] = both[0]
        pxb[1:4, :, cols] = both[1:4].astype(BF16)
        if n % 2 == 1:
            red.begin(n // 2)
    for k in range(2):
        red.rest(k)
    ahead()
    for k in range(2):
        red.pass_on(k)
    between()
    for k in range(2):
        red.end(k)


def vmem(*shape, dtype=BF16):
    return pltpu.VMEM(shape, dtype)


BACK = [
    vmem(4, 4 * OWN, 512),
    vmem(4, 4 * OWN, 512),
    vmem(4, OWN, D),
    vmem(3, OWN, D),
]


def params(cid):
    return pltpu.CompilerParams(
        collective_id=cid, has_side_effects=True, vmem_limit_bytes=60 * 1024 * 1024
    )


def body(
    residual_in, queries, keys, values, mix_lambda, head_gain, out_weight, norm_gain,
    gate_weight, up_weight, down_weight,
):
    whole = pl.BlockSpec(memory_space=pltpu.VMEM)
    hbm = pl.BlockSpec(memory_space=pl.ANY)
    smem = pl.BlockSpec(memory_space=pltpu.SMEM)
    return pl.pallas_call(
        layer_kernel,
        out_shape=jax.ShapeDtypeStruct((OWN, D), BF16),
        in_specs=[hbm] * 8 + [smem, whole, whole],
        out_specs=hbm,
        scratch_shapes=[
            vmem(4, TB, 256),
            vmem(2, 4, 2 * TB, VD),
            vmem(2, TB, 256),
            vmem(3, 2, 2, TB, 256),
            vmem(2, TB, 256),
            vmem(2, 4, VD + 16, 2 * TB, dtype=F32),
            vmem(2, 4, 8, 2 * TB, dtype=F32),
            vmem(2, 8, 2 * TB, dtype=F32),
            vmem(3, 2, 8, 2 * TB, dtype=F32),
            vmem(2, 4, VD, TB),
            vmem(2, 3, VD, TB),
            vmem(256, TB, dtype=F32),
            vmem(TB, 256),
            vmem(TB, 256),
            vmem(2, 4, OWN, D),
            vmem(OWN, D, dtype=F32),
            vmem(D, 2 * FL),
            vmem(D, FL),
            vmem(TB, 256),
            vmem(64, FL),
            vmem(64, FL),
            vmem(256, D),
            vmem(OWN, D),
            vmem(TB, FL),
            vmem(4, OWN, D, dtype=F32),
            *BACK,
            *BACK,
            vmem(OWN, D),
            pltpu.SemaphoreType.DMA((11,)),
            pltpu.SemaphoreType.DMA((160,)),
            pltpu.SemaphoreType.DMA((160,)),
        ],
        compiler_params=params(0),
        name="layer",
    )(
        queries, keys, values, residual_in, out_weight, gate_weight, up_weight, down_weight.T,
        mix_lambda, head_gain.reshape(1, VD), norm_gain.reshape(1, D),
    )


def solution(mesh):
    return jax.shard_map(
        body,
        mesh=mesh,
        in_specs=(
            P(("sp", "tp"), None),
            P("sp", "tp"),
            P("sp", "tp"),
            P("sp", "tp"),
            P("tp"),
            P(),
            P("tp", None),
            P(),
            P("sp", "tp"),
            P("sp", "tp"),
            P("tp", "sp"),
        ),
        out_specs=P(("sp", "tp"), None),
        check_vma=False,
    )
```
